32 devices in a mesh: st: 4 (over y, x), tp: 8 (over z, core).
Axes of the slice: x: 2, y: 2, z: 4, core: 2. Of those that a mesh axis runs over, the one named last changes fastest.
Arguments:
- tokens: bfloat16 [2048, 4096], P('st', 'tp'), may hold values from -6 to 6
- w_query: bfloat16 [4096, 2048], P(None, 'tp'), may hold values from -0.09375 to 0.09375
- w_key: bfloat16 [4096, 2048], P(None, 'tp'), may hold values from -0.09375 to 0.09375
- w_value: bfloat16 [4096, 4096], P(None, 'tp'), may hold values from -0.09375 to 0.09375
- w_mem_query: bfloat16 [4096, 2048], P(None, 'tp'), may hold values from -0.09375 to 0.09375
- w_mem_key: bfloat16 [4096, 2048], P(None, 'tp'), may hold values from -0.09375 to 0.09375
- w_mem_value: bfloat16 [4096, 2048], P(None, 'tp'), may hold values from -0.09375 to 0.09375
- w_gate: bfloat16 [4096, 16], P(None, 'tp'), may hold values from -0.09375 to 0.09375
- w_lift: bfloat16 [16, 128, 256], P('tp'), may hold values from -4 to 4
- decay_rate: float32 [16], P('tp'), may hold values from 0.000390625 to 0.1
- store: bfloat16 [512, 64, 4096], P('st', None, 'tp'), may hold values from -6 to 6
- passage_ids: int32 [16, 2], P('st'), may hold values from 0 to 511, as said below
Outputs:
- mixed: bfloat16 [2048, 4096], P('st', 'tp')
The draws below stay inside these ranges and needn't reach their ends.
Inputs may be any that keep to these rules, and one draw needn't show every extreme that they name: `passage_ids`: passage p is held by index p // 128 of st. Among the requests of the rows of one device along st, at most 4 name passages held by one index of st, and in every draw some index receives exactly 4 of them.
All inputs are finite; a program needn't handle non-finite values.
Results may differ from the reference program's by a relative error of at most 0.0095.
Values may be sent and summed in bfloat16 or wider, within the bound.
A program may use at most 64 MiB of HBM per device.

```python
import jax
import jax.numpy as jnp
from jax import lax

D = 4096
HEADS = 16
KEY_DIM = 128
VALUE_DIM = 256
MEM_DIM = 128
TOK_DEV = 512
SEQ_LEN = 512
RET_BLOCK = 64
BLOCK = 128
PICKS = 2
PASS_ROWS = 64
PASS_DEV = 128
CAP = 4
TOKENS = 2048
BLOCKS = 16
PASSAGES = 512
N_ST = 4


def draw_decay_rate(key, part):
    pick_key, slow_key, fast_key = jax.random.split(key, 3)
    quick = jax.random.uniform(pick_key, (HEADS,)) < 0.5
    slow_rate = jnp.exp(jax.random.uniform(slow_key, (HEADS,), minval=jnp.log(0.2 / SEQ_LEN), maxval=jnp.log(2.0 / SEQ_LEN)))
    fast_rate = jnp.exp(jax.random.uniform(fast_key, (HEADS,), minval=jnp.log(0.03), maxval=jnp.log(0.1)))
    return jnp.where(quick, fast_rate, slow_rate).astype(jnp.float32)


def draw_passage_ids(key, part):
    requests = TOK_DEV // BLOCK * PICKS
    slot_count = N_ST * CAP
    owners = jnp.repeat(jnp.arange(N_ST, dtype=jnp.int32), CAP)
    copies = jnp.tile(jnp.arange(CAP, dtype=jnp.int32), N_ST)

    def one_device(device):
        device_key = jax.random.fold_in(key, device)
        rank_key, shuffle_key, first_key, second_key = jax.random.split(device_key, 4)
        before = (device + N_ST - 1) % N_ST
        across = (device + N_ST // 2) % N_ST
        priority = jnp.where(owners == before, 0, jnp.where((owners == across) & (copies == 0), 1, 2))
        noise_rank = jax.random.randint(rank_key, (slot_count,), 0, 1 << 12)
        scores = priority * (1 << 24) + noise_rank * slot_count + jnp.arange(slot_count, dtype=jnp.int32)
        chosen = owners[jnp.argsort(scores)[:requests]]
        chosen = chosen[jax.random.permutation(shuffle_key, requests)]
        first_pick = jax.random.randint(first_key, (requests,), 0, PASS_DEV)
        second_pick = jax.random.randint(second_key, (requests,), 0, PASS_DEV)
        return chosen * PASS_DEV + jnp.minimum(first_pick, second_pick)
    drawn = jax.vmap(one_device)(jnp.arange(N_ST, dtype=jnp.int32))
    return drawn.reshape(BLOCKS, PICKS).astype(jnp.int32)


def block_scale(stream_key, extent, cuts, least, top_value):
    def one(dim, shards_of):
        heights = jax.random.uniform(jax.random.fold_in(jax.random.fold_in(stream_key, 6), dim), (shards_of,), jnp.float32, least / len(cuts), top_value / len(cuts))
        return jnp.repeat(jnp.exp(heights), extent[dim] // shards_of).reshape((-1,) + (1,) * (len(extent) - dim - 1))

    factor_of = one(*cuts[0])
    for cut in cuts[1:]:
        factor_of = factor_of * one(*cut)
    return factor_of


def noise(key, dims, scale, limit, cuts=(), held_as=jnp.bfloat16):
    entries = scale * jax.random.normal(key, dims, jnp.float32)
    if cuts:
        entries = entries * block_scale(key, dims, cuts, -0.22, 0.18)
    return jnp.clip(entries, -limit, limit).astype(held_as)


def setup_inputs(seed: int = 0) -> dict:
    streams_of = jax.random.split(jax.random.key(seed), 13)
    return {
        "tokens": noise(streams_of[0], (TOKENS, D), 1.0, 6.0, ((0, 4), (1, 8))),
        "w_query": noise(streams_of[1], (D, HEADS * KEY_DIM), D ** -0.5, 0.09375, ((1, 8),)),
        "w_key": noise(streams_of[2], (D, HEADS * KEY_DIM), D ** -0.5, 0.09375, ((1, 8),)),
        "w_value": noise(streams_of[3], (D, HEADS * VALUE_DIM), D ** -0.5, 0.09375, ((1, 8),)),
        "w_mem_query": noise(streams_of[4], (D, HEADS * MEM_DIM), D ** -0.5, 0.09375, ((1, 8),)),
        "w_mem_key": noise(streams_of[5], (D, HEADS * MEM_DIM), D ** -0.5, 0.09375, ((1, 8),)),
        "w_mem_value": noise(streams_of[6], (D, HEADS * MEM_DIM), D ** -0.5, 0.09375, ((1, 8),)),
        "w_gate": noise(streams_of[7], (D, HEADS), D ** -0.5, 0.09375, ((1, 8),)),
        "w_lift": noise(streams_of[8], (HEADS, MEM_DIM, VALUE_DIM), 0.7, 4.0, ((0, 8),)),
        "decay_rate": draw_decay_rate(jax.random.fold_in(streams_of[12], 71), 0),
        "store": noise(streams_of[10], (PASSAGES, PASS_ROWS, D), 1.0, 6.0, ((0, 4), (2, 8))),
        "passage_ids": draw_passage_ids(jax.random.fold_in(streams_of[12], 71), 0),
    }


norm_eps = 1e-06
rope_base = 10000.0

def rotate(values, positions):
    half_dim = values.shape[-1] // 2
    inverse = rope_base ** (-jnp.arange(half_dim, dtype=jnp.float32) / half_dim)
    angles = positions.astype(jnp.float32)[:, None] * inverse[None, :]
    cosine = jnp.cos(angles)[:, None, :]
    sine_table = jnp.sin(angles)[:, None, :]
    first_half = values[..., :half_dim]
    second_half = values[..., half_dim:]
    return jnp.concatenate([first_half * cosine - second_half * sine_table, first_half * sine_table + second_half * cosine], axis=-1)

def head_norm(values):
    return values * lax.rsqrt(lax.optimization_barrier(jnp.mean(values * values, axis=-1, keepdims=True)) + norm_eps)

def group_norm(values):
    centred = values - lax.optimization_barrier(jnp.mean(values, axis=-1, keepdims=True))
    return centred * lax.rsqrt(lax.optimization_barrier(jnp.mean(centred * centred, axis=-1, keepdims=True)) + norm_eps)

def retention(ret_query, ret_key, ret_value, rates, block_len):
    tokens_all, head_count, key_dim = ret_query.shape
    value_dim = ret_value.shape[-1]
    sequences = tokens_all // SEQ_LEN
    block_count = SEQ_LEN // block_len

    def blocked(array):
        shaped = array.astype(jnp.float32).reshape(sequences, block_count, block_len, head_count, array.shape[-1])
        return jnp.swapaxes(shaped, 0, 1)
    log_decay = -rates.astype(jnp.float32)
    offsets = jnp.arange(block_len, dtype=jnp.float32)
    decay_query = jnp.exp(log_decay[None, :] * (offsets[:, None] + 1.0))
    distance = offsets[:, None] - offsets[None, :]
    decay_mask = jnp.where(distance[None] >= 0.0, jnp.exp(log_decay[:, None, None] * jnp.maximum(distance, 0.0)[None]), 0.0)
    decay_key = jnp.exp(log_decay[None, :] * (block_len - 1.0 - offsets[:, None]))
    decay_block = jnp.exp(log_decay * block_len)
    highest = lax.Precision.HIGHEST

    def advance(memory_state, pieces):
        query_block, key_block, value_block = pieces
        carried = jnp.einsum('slhk,shkv->slhv', query_block, memory_state, precision=highest) * decay_query[None, :, :, None]
        scores = jnp.einsum('slhk,smhk->shlm', query_block, key_block, precision=highest) * decay_mask[None]
        within = jnp.einsum('shlm,smhv->slhv', scores, value_block, precision=highest)
        weighted = key_block * decay_key[None, :, :, None]
        memory_state = decay_block[None, :, None, None] * memory_state + jnp.einsum('slhk,slhv->shkv', weighted, value_block, precision=highest)
        return (memory_state, carried + within)
    initial = jnp.zeros((sequences, head_count, key_dim, value_dim), jnp.float32)
    _, outputs = lax.scan(advance, initial, (blocked(ret_query), blocked(ret_key), blocked(ret_value)))
    return jnp.swapaxes(outputs, 0, 1).reshape(tokens_all, head_count, value_dim)

def reference(tokens, w_query, w_key, w_value, w_mem_query, w_mem_key, w_mem_value, w_gate, w_lift, decay_rate, store, passage_ids):
    total_rows = tokens.shape[0]
    head_count = decay_rate.shape[0]
    highest = lax.Precision.HIGHEST
    features = tokens.astype(jnp.float32)
    row_scale = lax.rsqrt(lax.optimization_barrier(jnp.mean(features * features, axis=1, keepdims=True)) + norm_eps)
    positions = jnp.arange(total_rows, dtype=jnp.int32) % SEQ_LEN

    def project(weight):
        return jnp.dot(tokens, weight, preferred_element_type=jnp.float32)
    ret_query = rotate((project(w_query) * row_scale).reshape(total_rows, head_count, KEY_DIM), positions).astype(jnp.bfloat16)
    ret_key = (rotate((project(w_key) * row_scale).reshape(total_rows, head_count, KEY_DIM), positions) * KEY_DIM ** (-0.5)).astype(jnp.bfloat16)
    ret_value = (project(w_value) * row_scale).astype(jnp.bfloat16).reshape(total_rows, head_count, VALUE_DIM)
    mem_query = head_norm(project(w_mem_query).reshape(total_rows, head_count, MEM_DIM)).astype(jnp.bfloat16)
    gate_value = jax.nn.sigmoid(project(w_gate) * row_scale)
    ret_norm = group_norm(retention(ret_query, ret_key, ret_value, decay_rate, RET_BLOCK))

    def passage_rows(ident):
        passage = lax.dynamic_index_in_dim(store, ident, 0, keepdims=False)
        key_part = head_norm(jnp.dot(passage, w_mem_key, preferred_element_type=jnp.float32).reshape(PASS_ROWS, head_count, MEM_DIM))
        value_part = jnp.dot(passage, w_mem_value, preferred_element_type=jnp.float32).reshape(PASS_ROWS, head_count, MEM_DIM)
        return (key_part.astype(jnp.bfloat16), value_part.astype(jnp.bfloat16))
    pass_key, pass_value = lax.map(passage_rows, passage_ids.reshape(-1).astype(jnp.int32))
    block_count, picks = passage_ids.shape
    query_blocks = mem_query.reshape(block_count, BLOCK, head_count, MEM_DIM)
    key_blocks = pass_key.reshape(block_count, picks, PASS_ROWS, head_count, MEM_DIM)
    value_blocks = pass_value.reshape(block_count, picks, PASS_ROWS, head_count, MEM_DIM)

    def attend(pieces):
        query_block, key_block, value_block = pieces
        scores = jnp.einsum('thd,prhd->hptr', query_block.astype(jnp.float32), key_block.astype(jnp.float32), precision=highest) * MEM_DIM ** (-0.5)
        exponent = jnp.exp(scores)
        mass_sum = lax.optimization_barrier(jnp.sum(exponent, axis=3))
        rounded = lax.optimization_barrier(exponent.astype(jnp.bfloat16)).astype(jnp.float32)
        partial_value = jnp.einsum('hptr,prhd->pthd', rounded, value_block.astype(jnp.float32), precision=highest)
        partial_value = lax.optimization_barrier(partial_value.astype(jnp.bfloat16)).astype(jnp.float32)
        summed = lax.optimization_barrier(jnp.sum(partial_value, axis=0))
        return summed / jnp.swapaxes(lax.optimization_barrier(jnp.sum(mass_sum, axis=1)), 0, 1)[:, :, None]
    mem_out = lax.map(attend, (query_blocks, key_blocks, value_blocks)).reshape(total_rows, head_count, MEM_DIM).astype(jnp.bfloat16)
    mem_lift = jnp.einsum('thd,hde->the', mem_out.astype(jnp.float32), w_lift.astype(jnp.float32), precision=highest)
    mixed = (ret_norm + gate_value[:, :, None] * mem_lift).astype(jnp.bfloat16)
    return mixed.reshape(total_rows, head_count * VALUE_DIM)
```

```python
import functools

import jax
import jax.numpy as jnp
import numpy as np
from jax import lax
from jax.experimental import pallas as pl
from jax.experimental.pallas import tpu as pltpu
from jax.sharding import PartitionSpec as P

KEY_DIM = 128
VALUE_DIM = 256
MEM_DIM = 128
SEQ_LEN = 512
NORM_EPS = 1e-06
ROPE_BASE = 10000.0
CORES = 2
CHUNK = 128
MESH = pl.DeviceIdType.MESH
F32 = jnp.float32
BF16 = jnp.bfloat16


def dot(a, b):
    return jnp.dot(a, b, preferred_element_type=F32)


def dot_nt(a, b):
    return lax.dot_general(a, b, (((1,), (1,)), ((), ())), preferred_element_type=F32)


def kernel(
    n_st, n_tp, cap, picks, held,
    rate_ref, tok_hbm, wq_hbm, wk_hbm, wv_hbm, wm_hbm, wmk_hbm, wmv_hbm, wg_ref, lift_ref,
    cos_ref, sin_ref, store_hbm, ids_hbm,
    out_ref,
    tok, rows, wq, wk, wv, wm, wmk, wmv, store, slots, landed, ids_v, ids_s,
    acc_q, acc_k, acc_v, acc_m, acc_g, acc_s, acc_mk, acc_mv,
    rq, rk, rv, mq, ret, gate,
    load_sem, id_send, id_recv, pass_send, pass_recv,
    t_recv, t_send, t_left, t_pair, r_recv, r_send, r_left, r_pair,
):
    st = lax.axis_index("st")
    me = lax.axis_index("tp")
    z = me // CORES
    core = me % CORES
    n_z = n_tp // CORES
    total, cols = tok.shape[1:]
    heads = mq.shape[1] // MEM_DIM
    requests = ids_s.shape[2]
    pass_rows = store.shape[1]

    loads = []
    pairs = [(store_hbm, store), (ids_hbm, ids_v.at[st]), (tok_hbm, tok.at[me]), (wq_hbm, wq), (wk_hbm, wk),
             (wv_hbm, wv), (wm_hbm, wm), (wmk_hbm, wmk), (wmv_hbm, wmv)]
    for i, (src, dst) in enumerate(pairs):
        loads.append(pltpu.make_async_copy(src, dst, load_sem.at[i]))
        loads[-1].start()

    barrier = pltpu.get_barrier_semaphore()
    has_right = z < n_z - 1
    has_left = z > 0

    @pl.when(has_right)
    def _():
        pl.semaphore_signal(barrier, inc=1, device_id=(st, me + CORES), device_id_type=MESH)

    @pl.when(has_left)
    def _():
        pl.semaphore_signal(barrier, inc=1, device_id=(st, me - CORES), device_id_type=MESH)

    pair = z * CORES + (1 - core)
    pl.semaphore_signal(barrier, inc=1, device_id=(st, pair), device_id_type=MESH)
    for d in range(1, n_st):
        pl.semaphore_signal(barrier, inc=1, device_id=((st + d) % n_st, me), device_id_type=MESH)
    pl.semaphore_wait(barrier, n_st + has_right.astype(jnp.int32) + has_left.astype(jnp.int32))

    def remote(src, dst, send, recv, to_st, to_tp):
        return pltpu.make_async_remote_copy(
            src_ref=src, dst_ref=dst, send_sem=send, recv_sem=recv,
            device_id=(to_st, to_tp), device_id_type=MESH)

    def line(buf, sems):
        recv, send, left, pairing = sems

        def right_copy(j, src=None):
            return remote(buf.at[j] if src is None else src, buf.at[j], send.at[j], recv.at[j], st, me + CORES)

        def left_copy(j, src=None):
            sem = left.at[0] if src is not None else send.at[j]
            return remote(buf.at[j] if src is None else src, buf.at[j], sem, recv.at[j], st, me - CORES)

        def pair_copy(j, src=None):
            return remote(buf.at[j] if src is None else src, buf.at[j], pairing.at[j], recv.at[j], st, pair)

        def send_own(src):
            @pl.when(has_right)
            def _():
                right_copy(me, src).start()

            @pl.when(has_left)
            def _():
                left_copy(me, src).start()
            pair_copy(me, src).start()

        def relay(d):
            from_left = me - CORES * d
            from_right = me + CORES * d

            @pl.when(from_left >= 0)
            def _():
                pair_copy(from_left).wait_recv()

                @pl.when(has_right)
                def _():
                    right_copy(from_left).start()
                pair_copy(from_left).start()

            @pl.when(from_right < n_tp)
            def _():
                pair_copy(from_right).wait_recv()

                @pl.when(has_left)
                def _():
                    left_copy(from_right).start()
                pair_copy(from_right).start()

        def drain(src):
            @pl.when(has_right)
            def _():
                right_copy(me, src).wait_send()

            @pl.when(has_left)
            def _():
                left_copy(me, src).wait_send()
            pair_copy(me, src).wait_send()

            def step(d, carry):
                from_left = me - CORES * d
                from_right = me + CORES * d

                @pl.when(from_left >= 0)
                def _():
                    @pl.when(has_right)
                    def _():
                        right_copy(from_left).wait_send()
                    pair_copy(from_left).wait_send()

                @pl.when(from_right < n_tp)
                def _():
                    @pl.when(has_left)
                    def _():
                        left_copy(from_right).wait_send()
                    pair_copy(from_right).wait_send()
                return carry
            lax.fori_loop(1, n_z, step, 0)

        def consume(low, high, take):
            def step(q, carry):
                d, side, which = q // 4, (q // 2) % 2, q % 2
                at = z + (2 * side - 1) * d
                j = at * CORES + which
                valid = (at >= 0) & (at < n_z) & ((d > 0) | (side == 0))

                @pl.when(valid)
                def _():
                    @pl.when(which != core)
                    def _():
                        pair_copy(j).wait_recv()
                    take(j)
                return carry
            lax.fori_loop(4 * low, 4 * high, step, 0)

        return send_own, relay, drain, consume

    tok_send, tok_relay, tok_drain, tok_consume = line(tok, (t_recv, t_send, t_left, t_pair))
    row_send, row_relay, row_drain, row_consume = line(rows, (r_recv, r_send, r_left, r_pair))

    def id_copy(d):
        return remote(ids_hbm, ids_v.at[st], id_send.at[d], id_recv.at[st], (st + d) % n_st, me)

    def id_wait(d):
        other = (st + d) % n_st
        return remote(ids_hbm, ids_v.at[other], id_send.at[d], id_recv.at[other], other, me)

    for d in range(1, n_st):
        id_copy(d).start()
    tok_send(tok_hbm)

    for ref in (acc_q, acc_k, acc_v, acc_m, acc_g, acc_s, acc_mk, acc_mv):
        ref[...] = jnp.zeros_like(ref)

    loads[1].wait()
    for d in range(1, n_st):
        id_wait(d).wait_recv()
    to_scalar = pltpu.make_async_copy(ids_v, ids_s, load_sem.at[len(pairs)])
    to_scalar.start()
    to_scalar.wait()
    loads[0].wait()

    def asked(source, k):
        found = jnp.int32(0)
        seen = jnp.int32(0)
        for i in range(requests):
            ident = ids_s[source, 0, i]
            mine = (ident // held) == st
            found = jnp.where(mine & (seen == k), ident % held, found)
            seen = seen + mine.astype(jnp.int32)
        return found

    def fill(d, carry):
        source = (st + d) % n_st
        for k in range(cap):
            slots[d, k] = store[asked(source, k)]
        return carry
    lax.fori_loop(1, n_st, fill, 0)

    def pass_copy(d):
        return remote(slots.at[d], landed.at[st], pass_send.at[d], pass_recv.at[st], (st + d) % n_st, me)

    def pass_wait(d):
        other = (st + d) % n_st
        return remote(slots.at[d], landed.at[other], pass_send.at[d], pass_recv.at[other], other, me)

    for d in range(1, n_st):
        pass_copy(d).start()
    for k in range(cap):
        landed[st, k] = store[asked(st, k)]

    tok_relay(1)

    for d in range(1, n_st):
        pass_wait(d).wait_recv()
    for i in range(requests):
        ident = ids_s[st, 0, i]
        owner = ident // held
        order = jnp.int32(0)
        for e in range(i):
            order = order + ((ids_s[st, 0, e] // held) == owner).astype(jnp.int32)
        rows[me, pl.ds(i * pass_rows, pass_rows), :] = landed[owner, jnp.minimum(order, cap - 1)]
    row_send(None)

    for i in range(2, 9):
        loads[i].wait()

    def take_tokens(j):
        at = pl.ds(pl.multiple_of(j * cols, cols), cols)

        def part(c, carry):
            here = pl.ds(pl.multiple_of(c * 256, 256), 256)
            x = tok[j, here, :]
            acc_q[here, :] += dot(x, wq[at, :])
            acc_k[here, :] += dot(x, wk[at, :])
            acc_v[here, :] += dot(x, wv[at, :])
            acc_m[here, :] += dot(x, wm[at, :])
            wide = x.astype(F32)
            if heads > 1:
                acc_g[here, :] += dot_nt(x, wg_ref[:, at])
            else:
                acc_g[here, :] += jnp.sum(wide * wg_ref[:, at].astype(F32), axis=1, keepdims=True)
            squares = acc_s[here, :]
            for piece in range(cols // 128):
                slab = wide[:, piece * 128:(piece + 1) * 128]
                squares = squares + slab * slab
            acc_s[here, :] = squares
            return carry
        lax.fori_loop(0, total // 256, part, 0)

    tok_consume(0, 2, take_tokens)

    def token_stage(d, carry):
        tok_relay(d)
        tok_consume(d, d + 1, take_tokens)
        return carry
    lax.fori_loop(2, n_z, token_stage, 0)

    row_relay(1)

    def prepare(c, carry):
        here = pl.ds(pl.multiple_of(c * CHUNK, CHUNK), CHUNK)
        scale = lax.rsqrt(jnp.sum(acc_s[here, :], axis=1, keepdims=True) / (n_tp * cols) + NORM_EPS)
        cosine, sine = cos_ref[here, :], sin_ref[here, :]

        def rotate(v):
            return v * cosine + pltpu.roll(v, KEY_DIM // 2, 1) * sine
        for h in range(heads):
            at = slice(h * KEY_DIM, (h + 1) * KEY_DIM)
            rq[here, at] = rotate(acc_q[here, at] * scale).astype(BF16)
            rk[here, at] = (rotate(acc_k[here, at] * scale) * KEY_DIM ** (-0.5)).astype(BF16)
            m = acc_m[here, at]
            mq[here, at] = (m * lax.rsqrt(jnp.mean(m * m, axis=1, keepdims=True) + NORM_EPS)).astype(BF16)
        rv[here, :] = (acc_v[here, :] * scale).astype(BF16)
        gate[here, :] = jax.nn.sigmoid(acc_g[here, :] * scale)
        return carry
    lax.fori_loop(0, total // CHUNK, prepare, 0)

    def retain(c, carry):
        here = pl.ds(pl.multiple_of(c * CHUNK, CHUNK), CHUNK)
        start = (c * CHUNK) // SEQ_LEN * SEQ_LEN
        whole = pl.ds(pl.multiple_of(start, SEQ_LEN), SEQ_LEN)
        t = lax.broadcasted_iota(jnp.int32, (CHUNK, SEQ_LEN), 0) + (c * CHUNK - start)
        s = lax.broadcasted_iota(jnp.int32, (CHUNK, SEQ_LEN), 1)
        gap = (t - s).astype(F32)
        for h in range(heads):
            at = slice(h * KEY_DIM, (h + 1) * KEY_DIM)
            wide = slice(h * VALUE_DIM, (h + 1) * VALUE_DIM)
            decay = jnp.where(gap >= 0.0, jnp.exp(-rate_ref[h] * jnp.maximum(gap, 0.0)), 0.0)
            scores = dot_nt(rq[here, at], rk[whole, at]) * decay
            upper = scores.astype(BF16)
            lower = (scores - upper.astype(F32)).astype(BF16)
            value = rv[whole, wide]
            o = dot(upper, value) + dot(lower, value)
            o = o - jnp.mean(o, axis=1, keepdims=True)
            ret[here, wide] = o * lax.rsqrt(jnp.mean(o * o, axis=1, keepdims=True) + NORM_EPS)
        return carry
    lax.fori_loop(0, total // CHUNK, retain, 0)

    def take_rows(j):
        at = pl.ds(pl.multiple_of(j * cols, cols), cols)

        def part(c, carry):
            here = pl.ds(pl.multiple_of(c * 256, 256), 256)
            x = rows[j, here, :]
            acc_mk[here, :] += dot(x, wmk[at, :])
            acc_mv[here, :] += dot(x, wmv[at, :])
            return carry
        lax.fori_loop(0, rows.shape[1] // 256, part, 0)

    row_consume(0, 2, take_rows)

    def row_stage(d, carry):
        row_relay(d)
        row_consume(d, d + 1, take_rows)
        return carry
    lax.fori_loop(2, n_z, row_stage, 0)

    blocks = requests // picks
    block = total // blocks
    keys = picks * pass_rows

    def attend(b, carry):
        here = pl.ds(pl.multiple_of(b * block, block), block)
        there = pl.ds(pl.multiple_of(b * keys, keys), keys)
        for h in range(heads):
            at = slice(h * MEM_DIM, (h + 1) * MEM_DIM)
            wide = slice(h * VALUE_DIM, (h + 1) * VALUE_DIM)
            k = acc_mk[there, at]
            k = (k * lax.rsqrt(jnp.mean(k * k, axis=1, keepdims=True) + NORM_EPS)).astype(BF16)
            v = acc_mv[there, at].astype(BF16)
            exponent = jnp.exp(dot_nt(mq[here, at], k) * MEM_DIM ** (-0.5))
            mass = jnp.sum(exponent, axis=1, keepdims=True)
            o = (dot(exponent.astype(BF16), v) / mass).astype(BF16)
            lifted = dot(o, lift_ref[h])
            out_ref[here, wide] = (ret[here, wide] + gate[here, h:h + 1] * lifted).astype(BF16)
        return carry
    lax.fori_loop(0, blocks, attend, 0)

    for d in range(1, n_st):
        id_copy(d).wait_send()
        pass_copy(d).wait_send()
    tok_drain(tok_hbm)
    row_drain(None)


def rotary_tables(total):
    half = KEY_DIM // 2
    angle = (np.arange(total) % SEQ_LEN)[:, None] * ROPE_BASE ** (-np.arange(half) / half)[None, :]
    cosine, sine = np.cos(angle), np.sin(angle)
    return (np.concatenate([cosine, cosine], 1).astype(np.float32),
            np.concatenate([-sine, sine], 1).astype(np.float32))


def solution(mesh):
    n_st, n_tp = mesh.shape["st"], mesh.shape["tp"]

    def per_device(tokens, w_query, w_key, w_value, w_mem_query, w_mem_key, w_mem_value, w_gate, w_lift,
                   decay_rate, store, passage_ids):
        total, cols = tokens.shape
        heads = decay_rate.shape[0]
        blocks, picks = passage_ids.shape
        requests = blocks * picks
        held, pass_rows, _ = store.shape
        cap = max(1, 2 * requests // n_st)
        cosine, sine = rotary_tables(total)
        hbm = pl.BlockSpec(memory_space=pl.ANY)
        vmem = pl.BlockSpec(memory_space=pltpu.VMEM)
        smem = pl.BlockSpec(memory_space=pltpu.SMEM)
        V = pltpu.VMEM
        dma = pltpu.SemaphoreType.DMA
        wide = w_value.shape[1]
        key_cols, mem_cols = w_query.shape[1], w_mem_query.shape[1]
        scratch = [
            V((n_tp, total, cols), BF16), V((n_tp, requests * pass_rows, cols), BF16),
            V(w_query.shape, BF16), V(w_key.shape, BF16), V(w_value.shape, BF16),
            V(w_mem_query.shape, BF16), V(w_mem_key.shape, BF16), V(w_mem_value.shape, BF16),
            V(store.shape, BF16), V((n_st, cap, pass_rows, cols), BF16), V((n_st, cap, pass_rows, cols), BF16),
            V((n_st, 1, requests), jnp.int32), pltpu.SMEM((n_st, 1, requests), jnp.int32),
            V((total, key_cols), F32), V((total, key_cols), F32), V((total, wide), F32), V((total, mem_cols), F32),
            V((total, heads), F32), V((total, 128), F32),
            V((requests * pass_rows, mem_cols), F32), V((requests * pass_rows, mem_cols), F32),
            V((total, key_cols), BF16), V((total, key_cols), BF16), V((total, wide), BF16), V((total, mem_cols), BF16),
            V((total, wide), F32), V((total, heads), F32),
            dma((10,)), dma((n_st,)), dma((n_st,)), dma((n_st,)), dma((n_st,)),
            dma((n_tp,)), dma((n_tp,)), dma((1,)), dma((n_tp,)),
            dma((n_tp,)), dma((n_tp,)), dma((1,)), dma((n_tp,)),
        ]
        return pl.pallas_call(
            functools.partial(kernel, n_st, n_tp, cap, picks, held),
            out_shape=jax.ShapeDtypeStruct((total, heads * VALUE_DIM), BF16),
            in_specs=[smem] + [hbm] * 7 + [vmem] * 4 + [hbm] * 2,
            out_specs=vmem,
            scratch_shapes=scratch,
            compiler_params=pltpu.CompilerParams(
                collective_id=0, has_side_effects=True, vmem_limit_bytes=60 * 1024 * 1024),
        )(decay_rate, tokens, w_query, w_key, w_value, w_mem_query, w_mem_key, w_mem_value,
          w_gate.T, w_lift, jnp.asarray(cosine), jnp.asarray(sine), store, passage_ids.reshape(1, requests))

    in_specs = (P("st", "tp"),) + (P(None, "tp"),) * 7 + (
        P("tp", None, None), P("tp"), P("st", None, "tp"), P("st", None))
    return jax.shard_map(per_device, mesh=mesh, in_specs=in_specs, out_specs=P("st", "tp"), check_vma=False)
```

```python
import functools

import jax
import jax.numpy as jnp
import numpy as np
from jax import lax
from jax.experimental import pallas as pl
from jax.experimental.pallas import tpu as pltpu
from jax.sharding import PartitionSpec as P

KEY_DIM = 128
VALUE_DIM = 256
MEM_DIM = 128
SEQ_LEN = 512
NORM_EPS = 1e-06
ROPE_BASE = 10000.0
CORES = 2
CHUNK = 128
PIECES = 2
SPLIT = 1
MESH = pl.DeviceIdType.MESH
F32 = jnp.float32
BF16 = jnp.bfloat16


def dot(a, b):
    return jnp.dot(a, b, preferred_element_type=F32)


def dot_nt(a, b):
    return lax.dot_general(a, b, (((1,), (1,)), ((), ())), preferred_element_type=F32)


def kernel(
    n_st, n_tp, cap, picks, held,
    rate_ref, tok_hbm, wq_hbm, wk_hbm, wv_hbm, wm_hbm, wmk_hbm, wmv_hbm, wg_ref, lift_hbm,
    cos_hbm, sin_hbm, store_hbm, ids_hbm,
    out_ref,
    tok, rows, cos_ref, sin_ref, lift_ref, wq, wk, wv, wm, wmk, wmv, store, slots, landed, ids_v, ids_s,
    acc_q, acc_k, acc_v, acc_m, acc_g, acc_s, acc_mk, acc_mv,
    rq, rk, rv, mq, ret, gate,
    load_sem, id_send, id_recv, pass_send, pass_recv,
    t_recv, t_send, t_left, t_pair, r_recv, r_send, r_left, r_pair,
):
    st = lax.axis_index("st")
    me = lax.axis_index("tp")
    z = me // CORES
    core = me % CORES
    n_z = n_tp // CORES
    total, cols = tok.shape[1:]
    heads = mq.shape[1] // MEM_DIM
    requests = ids_s.shape[1] * ids_s.shape[2]
    pass_rows = store.shape[1]

    loads = []
    pairs = [(store_hbm, store), (ids_hbm, ids_v.at[st]), (tok_hbm, tok.at[me]), (wq_hbm, wq), (wk_hbm, wk),
             (wv_hbm, wv), (wm_hbm, wm), (wmk_hbm, wmk), (wmv_hbm, wmv),
             (cos_hbm, cos_ref), (sin_hbm, sin_ref), (lift_hbm, lift_ref)]
    for i, (src, dst) in enumerate(pairs):
        loads.append(pltpu.make_async_copy(src, dst, load_sem.at[i]))
    loads[1].start()

    barrier = pltpu.get_barrier_semaphore()
    has_right = z < n_z - 1
    has_left = z > 0

    @pl.when(has_right)
    def _():
        pl.semaphore_signal(barrier, inc=1, device_id=(st, me + CORES), device_id_type=MESH)

    @pl.when(has_left)
    def _():
        pl.semaphore_signal(barrier, inc=1, device_id=(st, me - CORES), device_id_type=MESH)

    pair = z * CORES + (1 - core)
    pl.semaphore_signal(barrier, inc=1, device_id=(st, pair), device_id_type=MESH)
    for d in range(1, n_st):
        pl.semaphore_signal(barrier, inc=1, device_id=((st + d) % n_st, me), device_id_type=MESH)
    pl.semaphore_wait(barrier, n_st + has_right.astype(jnp.int32) + has_left.astype(jnp.int32))

    def remote(src, dst, send, recv, to_st, to_tp):
        return pltpu.make_async_remote_copy(
            src_ref=src, dst_ref=dst, send_sem=send, recv_sem=recv,
            device_id=(to_st, to_tp), device_id_type=MESH)

    def line(buf, sems):
        recv, send, left, pairing = sems
        size = buf.shape[1] // PIECES

        def piece(j, p):
            return buf.at[j, pl.ds(p * size, size)]

        def own_piece(src, p):
            return piece(me, p) if src is None else src.at[pl.ds(p * size, size)]

        def right_copy(j, p, src=None):
            return remote(piece(j, p) if src is None else src, piece(j, p), send.at[j, p], recv.at[j, p],
                          st, me + CORES)

        def left_copy(j, p, src=None):
            sem = left.at[0, p] if src is not None else send.at[j, p]
            return remote(piece(j, p) if src is None else src, piece(j, p), sem, recv.at[j, p], st, me - CORES)

        def pair_copy(j, p, src=None):
            return remote(piece(j, p) if src is None else src, piece(j, p), pairing.at[j, p], recv.at[j, p], st, pair)

        def send_own(src):
            for p in range(PIECES):
                own = own_piece(src, p)

                @pl.when(has_right)
                def _():
                    right_copy(me, p, own).start()

                @pl.when(has_left)
                def _():
                    left_copy(me, p, own).start()
            for p in range(PIECES):
                pair_copy(me, p, own_piece(src, p)).start()

        def relay(d, p):
            from_left = me - CORES * d
            from_right = me + CORES * d

            @pl.when(from_left >= 0)
            def _():
                pair_copy(from_left, p).wait_recv()

                @pl.when(has_right)
                def _():
                    right_copy(from_left, p).start()
                pair_copy(from_left, p).start()

            @pl.when(from_right < n_tp)
            def _():
                pair_copy(from_right, p).wait_recv()

                @pl.when(has_left)
                def _():
                    left_copy(from_right, p).start()
                pair_copy(from_right, p).start()

        def drain(src):
            def step(q, carry):
                d, p = q // PIECES, q % PIECES
                from_left = me - CORES * d
                from_right = me + CORES * d

                @pl.when(from_left >= 0)
                def _():
                    @pl.when(has_right)
                    def _():
                        right_copy(from_left, p).wait_send()
                    pair_copy(from_left, p).wait_send()

                @pl.when((d > 0) & (from_right < n_tp))
                def _():
                    @pl.when(has_left)
                    def _():
                        left_copy(from_right, p).wait_send()
                    pair_copy(from_right, p).wait_send()
                return carry
            for p in range(PIECES):
                @pl.when(has_left)
                def _():
                    left_copy(me, p, own_piece(src, p)).wait_send()
            lax.fori_loop(0, PIECES * n_z, step, 0)

        def consume(low, high, take, p):
            def step(q, carry):
                d, side, which = q // 4, (q // 2) % 2, q % 2
                at = z + (2 * side - 1) * d
                j = at * CORES + which
                valid = (at >= 0) & (at < n_z) & ((d > 0) | (side == 0))

                @pl.when(valid)
                def _():
                    @pl.when(which != core)
                    def _():
                        pair_copy(j, p).wait_recv()
                    take(j, p)
                return carry
            lax.fori_loop(4 * low, 4 * high, step, 0)

        return send_own, relay, drain, consume

    tok_send, tok_relay, tok_drain, tok_consume = line(tok, (t_recv, t_send, t_left, t_pair))
    row_send, row_relay, row_drain, row_consume = line(rows, (r_recv, r_send, r_left, r_pair))

    def id_copy(d):
        return remote(ids_hbm, ids_v.at[st], id_send.at[d], id_recv.at[st], (st + d) % n_st, me)

    def id_wait(d):
        other = (st + d) % n_st
        return remote(ids_hbm, ids_v.at[other], id_send.at[d], id_recv.at[other], other, me)

    for d in range(1, n_st):
        id_copy(d).start()
    tok_send(tok_hbm)
    loads[0].start()
    loads[2].start()

    for ref in (acc_q, acc_k, acc_v, acc_m, acc_g, acc_s, acc_mk, acc_mv):
        ref[...] = jnp.zeros_like(ref)

    loads[1].wait()
    for d in range(1, n_st):
        id_wait(d).wait_recv()
    to_scalar = pltpu.make_async_copy(ids_v, ids_s, load_sem.at[len(pairs)])
    to_scalar.start()
    to_scalar.wait()
    loads[0].wait()

    def asked(source, k):
        found = jnp.int32(0)
        seen = jnp.int32(0)
        for i in range(requests):
            ident = ids_s[source, i % picks, i // picks]
            mine = (ident // held) == st
            found = jnp.where(mine & (seen == k), ident % held, found)
            seen = seen + mine.astype(jnp.int32)
        return found

    def fill(d, carry):
        source = (st + d) % n_st
        for k in range(cap):
            slots[d, k] = store[asked(source, k)]
        return carry
    lax.fori_loop(1, n_st, fill, 0)

    def pass_copy(d):
        return remote(slots.at[d], landed.at[st], pass_send.at[d], pass_recv.at[st], (st + d) % n_st, me)

    def pass_wait(d):
        other = (st + d) % n_st
        return remote(slots.at[d], landed.at[other], pass_send.at[d], pass_recv.at[other], other, me)

    for d in range(1, n_st):
        pass_copy(d).start()
    for k in range(cap):
        landed[st, k] = store[asked(st, k)]
    for i in range(3, len(pairs)):
        loads[i].start()

    for p in range(PIECES):
        tok_relay(1, p)

    for d in range(1, n_st):
        pass_wait(d).wait_recv()
    for i in range(requests):
        ident = ids_s[st, i % picks, i // picks]
        owner = ident // held
        order = jnp.int32(0)
        for e in range(i):
            order = order + ((ids_s[st, e % picks, e // picks] // held) == owner).astype(jnp.int32)
        rows[me, pl.ds(i * pass_rows, pass_rows), :] = landed[owner, jnp.minimum(order, cap - 1)]
    row_send(None)

    for i in range(2, len(pairs)):
        loads[i].wait()

    def take_tokens(j, p):
        at = pl.ds(pl.multiple_of(j * cols, cols), cols)
        step_rows = total // PIECES // SPLIT

        def part(c, carry):
            here = pl.ds(pl.multiple_of((p * SPLIT + c) * step_rows, step_rows), step_rows)
            x = tok[j, here, :]
            acc_q[here, :] += dot(x, wq[at, :])
            acc_k[here, :] += dot(x, wk[at, :])
            acc_v[here, :] += dot(x, wv[at, :])
            acc_m[here, :] += dot(x, wm[at, :])
            wide = x.astype(F32)
            if heads > 1:
                acc_g[here, :] += dot_nt(x, wg_ref[:, at])
            else:
                acc_g[here, :] += jnp.sum(wide * wg_ref[:, at].astype(F32), axis=1, keepdims=True)
            squares = acc_s[here, :]
            for piece in range(cols // 128):
                slab = wide[:, piece * 128:(piece + 1) * 128]
                squares = squares + slab * slab
            acc_s[here, :] = squares
            return carry
        lax.fori_loop(0, SPLIT, part, 0)

    def token_piece(p, carry):
        tok_consume(0, 2, take_tokens, p)
        return carry
    lax.fori_loop(0, PIECES, token_piece, 0)

    def token_stage(q, carry):
        d, p = q // PIECES, q % PIECES
        tok_relay(d, p)
        tok_consume(d, d + 1, take_tokens, p)
        return carry
    lax.fori_loop(2 * PIECES, n_z * PIECES, token_stage, 0)

    for p in range(PIECES):
        row_relay(1, p)

    def prepare(c, carry):
        here = pl.ds(pl.multiple_of(c * CHUNK, CHUNK), CHUNK)
        scale = lax.rsqrt(jnp.sum(acc_s[here, :], axis=1, keepdims=True) / (n_tp * cols) + NORM_EPS)
        cosine, sine = cos_ref[here, :], sin_ref[here, :]

        def rotate(v):
            return v * cosine + pltpu.roll(v, KEY_DIM // 2, 1) * sine
        for h in range(heads):
            at = slice(h * KEY_DIM, (h + 1) * KEY_DIM)
            rq[here, at] = rotate(acc_q[here, at] * scale).astype(BF16)
            rk[here, at] = (rotate(acc_k[here, at] * scale) * KEY_DIM ** (-0.5)).astype(BF16)
            m = acc_m[here, at]
            mq[here, at] = (m * lax.rsqrt(jnp.mean(m * m, axis=1, keepdims=True) + NORM_EPS)).astype(BF16)
        rv[here, :] = (acc_v[here, :] * scale).astype(BF16)
        gate[here, :] = jax.nn.sigmoid(acc_g[here, :] * scale)
        return carry
    lax.fori_loop(0, total // CHUNK, prepare, 0)

    def retain(c, carry):
        here = pl.ds(pl.multiple_of(c * CHUNK, CHUNK), CHUNK)
        start = (c * CHUNK) // SEQ_LEN * SEQ_LEN
        whole = pl.ds(pl.multiple_of(start, SEQ_LEN), SEQ_LEN)
        t = lax.broadcasted_iota(jnp.int32, (CHUNK, SEQ_LEN), 0) + (c * CHUNK - start)
        s = lax.broadcasted_iota(jnp.int32, (CHUNK, SEQ_LEN), 1)
        gap = (t - s).astype(F32)
        for h in range(heads):
            at = slice(h * KEY_DIM, (h + 1) * KEY_DIM)
            wide = slice(h * VALUE_DIM, (h + 1) * VALUE_DIM)
            decay = jnp.where(gap >= 0.0, jnp.exp(-rate_ref[h] * jnp.maximum(gap, 0.0)), 0.0)
            scores = dot_nt(rq[here, at], rk[whole, at]) * decay
            upper = scores.astype(BF16)
            lower = (scores - upper.astype(F32)).astype(BF16)
            value = rv[whole, wide]
            o = dot(upper, value) + dot(lower, value)
            o = o - jnp.mean(o, axis=1, keepdims=True)
            ret[here, wide] = o * lax.rsqrt(jnp.mean(o * o, axis=1, keepdims=True) + NORM_EPS)
        return carry
    lax.fori_loop(0, total // CHUNK, retain, 0)

    def take_rows(j, p):
        at = pl.ds(pl.multiple_of(j * cols, cols), cols)
        size = rows.shape[1] // PIECES
        here = pl.ds(pl.multiple_of(p * size, size), size)
        x = rows[j, here, :]
        acc_mk[here, :] += dot(x, wmk[at, :])
        acc_mv[here, :] += dot(x, wmv[at, :])

    def row_piece(p, carry):
        row_consume(0, 2, take_rows, p)
        return carry
    lax.fori_loop(0, PIECES, row_piece, 0)

    blocks = requests // picks
    block = total // blocks
    keys = picks * pass_rows

    def attend(b, carry):
        here = pl.ds(pl.multiple_of(b * block, block), block)
        there = pl.ds(pl.multiple_of(b * keys, keys), keys)
        for h in range(heads):
            at = slice(h * MEM_DIM, (h + 1) * MEM_DIM)
            wide = slice(h * VALUE_DIM, (h + 1) * VALUE_DIM)
            k = acc_mk[there, at]
            k = (k * lax.rsqrt(jnp.mean(k * k, axis=1, keepdims=True) + NORM_EPS)).astype(BF16)
            v = acc_mv[there, at].astype(BF16)
            exponent = jnp.exp(dot_nt(mq[here, at], k) * MEM_DIM ** (-0.5))
            mass = jnp.sum(exponent, axis=1, keepdims=True)
            o = (dot(exponent.astype(BF16), v) / mass).astype(BF16)
            lifted = dot(o, lift_ref[h])
            out_ref[here, wide] = (ret[here, wide] + gate[here, h:h + 1] * lifted).astype(BF16)
        return carry
    def row_stage(q, carry):
        d, p = q // PIECES, q % PIECES
        row_relay(d, p)
        row_consume(d, d + 1, take_rows, p)

        @pl.when(d == n_z - 1)
        def _():
            share = blocks // PIECES
            lax.fori_loop(p * share, (p + 1) * share, attend, 0)
        return carry
    lax.fori_loop(2 * PIECES, n_z * PIECES, row_stage, 0)

    for d in range(1, n_st):
        id_copy(d).wait_send()
        pass_copy(d).wait_send()
    tok_drain(tok_hbm)
    row_drain(None)


def rotary_tables(total):
    half = KEY_DIM // 2
    angle = (np.arange(total) % SEQ_LEN)[:, None] * ROPE_BASE ** (-np.arange(half) / half)[None, :]
    cosine, sine = np.cos(angle), np.sin(angle)
    return (np.concatenate([cosine, cosine], 1).astype(np.float32),
            np.concatenate([-sine, sine], 1).astype(np.float32))


def solution(mesh):
    n_st, n_tp = mesh.shape["st"], mesh.shape["tp"]

    def per_device(tokens, w_query, w_key, w_value, w_mem_query, w_mem_key, w_mem_value, w_gate, w_lift,
                   decay_rate, store, passage_ids):
        total, cols = tokens.shape
        heads = decay_rate.shape[0]
        blocks, picks = passage_ids.shape
        requests = blocks * picks
        held, pass_rows, _ = store.shape
        cap = max(1, 2 * requests // n_st)
        cosine, sine = rotary_tables(total)
        hbm = pl.BlockSpec(memory_space=pl.ANY)
        vmem = pl.BlockSpec(memory_space=pltpu.VMEM)
        smem = pl.BlockSpec(memory_space=pltpu.SMEM)
        V = pltpu.VMEM
        dma = pltpu.SemaphoreType.DMA
        wide = w_value.shape[1]
        key_cols, mem_cols = w_query.shape[1], w_mem_query.shape[1]
        scratch = [
            V((n_tp, total, cols), BF16), V((n_tp, requests * pass_rows, cols), BF16),
            V(cosine.shape, F32), V(sine.shape, F32), V(w_lift.shape, BF16),
            V(w_query.shape, BF16), V(w_key.shape, BF16), V(w_value.shape, BF16),
            V(w_mem_query.shape, BF16), V(w_mem_key.shape, BF16), V(w_mem_value.shape, BF16),
            V(store.shape, BF16), V((n_st, cap, pass_rows, cols), BF16), V((n_st, cap, pass_rows, cols), BF16),
            V((n_st, picks, blocks), jnp.int32), pltpu.SMEM((n_st, picks, blocks), jnp.int32),
            V((total, key_cols), F32), V((total, key_cols), F32), V((total, wide), F32), V((total, mem_cols), F32),
            V((total, heads), F32), V((total, 128), F32),
            V((requests * pass_rows, mem_cols), F32), V((requests * pass_rows, mem_cols), F32),
            V((total, key_cols), BF16), V((total, key_cols), BF16), V((total, wide), BF16), V((total, mem_cols), BF16),
            V((total, wide), F32), V((total, heads), F32),
            dma((16,)), dma((n_st,)), dma((n_st,)), dma((n_st,)), dma((n_st,)),
            dma((n_tp, PIECES)), dma((n_tp, PIECES)), dma((1, PIECES)), dma((n_tp, PIECES)),
            dma((n_tp, PIECES)), dma((n_tp, PIECES)), dma((1, PIECES)), dma((n_tp, PIECES)),
        ]
        return pl.pallas_call(
            functools.partial(kernel, n_st, n_tp, cap, picks, held),
            out_shape=jax.ShapeDtypeStruct((total, heads * VALUE_DIM), BF16),
            in_specs=[smem] + [hbm] * 7 + [vmem] + [hbm] * 5,
            out_specs=vmem,
            scratch_shapes=scratch,
            compiler_params=pltpu.CompilerParams(
                collective_id=0, has_side_effects=True, vmem_limit_bytes=60 * 1024 * 1024),
        )(decay_rate, tokens, w_query, w_key, w_value, w_mem_query, w_mem_key, w_mem_value,
          w_gate.T, w_lift, jnp.asarray(cosine), jnp.asarray(sine), store, passage_ids.T)

    in_specs = (P("st", "tp"),) + (P(None, "tp"),) * 7 + (
        P("tp", None, None), P("tp"), P("st", None, "tp"), P("st", None))
    return jax.shard_map(per_device, mesh=mesh, in_specs=in_specs, out_specs=P("st", "tp"), check_vma=False)
```
